32 devices in a mesh: fs: 16 (over z, y, core), tp: 2 (over x).
Axes of the slice: x: 2, y: 2, z: 4, core: 2. Of those that a mesh axis runs over, the one named last changes fastest.
Arguments:
- saved_input: bfloat16 [8192, 3072], P('fs'), may hold values from -6 to 6
- output_cotangent: bfloat16 [8192, 3072], P('fs'), may hold values from -6 to 6
- recurrent_output: bfloat16 [8192, 1536], P('fs', 'tp'), may hold values from -6 to 6
- forget_logit: bfloat16 [8192, 1536], P('fs', 'tp'), may hold values from -12 to 12
- forget_cotangent: bfloat16 [8192, 1536], P('fs', 'tp'), may hold values from -6 to 6
- lower_bound: float32 [1536], P('tp'), may hold values from 0.2 to 0.9
- basis_in: bfloat16 [3072, 384], P('fs'), may hold values from -1.2629537 to 1.2629537
- basis_out: bfloat16 [3072, 384], P('fs'), may hold values from -1.2629537 to 1.2629537
- moment_in: float32 [384, 1536], P('fs', 'tp'), may hold values from -6 to 6
- second_in: float32 [384, 1536], P('fs', 'tp'), may hold values from 0.25 to 4
- moment_out: float32 [384, 1536], P('fs', 'tp'), may hold values from -6 to 6
- second_out: float32 [384, 1536], P('fs', 'tp'), may hold values from 0.25 to 4
- weight_in: float32 [3072, 1536], P('fs', 'tp'), may hold values from -0.109375 to 0.109375
- weight_out: float32 [1536, 3072], P('tp', 'fs'), may hold values from -0.15625 to 0.15625
Outputs:
- moment_in_new: float32 [384, 1536], P('fs', 'tp')
- second_in_new: float32 [384, 1536], P('fs', 'tp')
- moment_out_new: float32 [384, 1536], P('fs', 'tp')
- second_out_new: float32 [384, 1536], P('fs', 'tp')
- weight_in_new: float32 [3072, 1536], P('fs', 'tp')
- weight_out_new: float32 [1536, 3072], P('tp', 'fs')
- copy_in: bfloat16 [3072, 1536], P(None, 'tp')
- copy_out: bfloat16 [1536, 3072], P('tp')
The draws below stay inside these ranges and needn't reach their ends.
All inputs are finite; a program needn't handle non-finite values.
Results may differ from the reference program's by a relative error of at most 0.0023.
Values may be sent and summed in bfloat16 or wider, within the bound.
A program may use at most 64 MiB of HBM per device.

```python
import math
import jax
import jax.numpy as jnp
from jax import lax

D = 3072
HW = 1536
R = 384
TOKENS = 8192


def scaled_basis(key):
    first, second = jax.random.split(key)
    ramp = 10.0 ** (jnp.arange(R, dtype=jnp.float32) / R)
    jitter = jax.random.uniform(first, (R,), jnp.float32, 0.7, 1.4)
    values = jnp.clip(jax.random.normal(second, (D, R), jnp.float32), -5.0, 5.0)
    return (values * ramp[None, :] * jitter[None, :] * D ** (-0.5)).astype(jnp.bfloat16)


def draw_basis_in(key, part):
    return scaled_basis(jax.random.fold_in(key, 11))


def draw_basis_out(key, part):
    return scaled_basis(jax.random.fold_in(key, 23))


def levels(rng, shape, cuts, smallest, top_value):
    level = 1.0
    for position, blocks in cuts:
        steps = jax.random.uniform(jax.random.fold_in(jax.random.fold_in(rng, 6), position), (blocks,), jnp.float32, smallest / len(cuts), top_value / len(cuts))
        level = level * jnp.repeat(jnp.exp(steps), shape[position] // blocks).reshape((-1,) + (1,) * (len(shape) - 1 - position))
    return level


def centred(key, extent, scale, most, cuts=(), held_as=jnp.bfloat16):
    values = jax.random.normal(key, extent, jnp.float32) * scale
    if len(cuts) > 0:
        values = levels(key, extent, cuts, -0.22, 0.18) * values
    return jnp.clip(values, min=-most, max=most).astype(held_as)


def setup_inputs(seed: int = 0) -> dict:
    key_of = jax.random.split(jax.random.key(seed), 15)
    saved_input = centred(key_of[0], (TOKENS, D), 1.0, 6.0, ((0, 16),))
    output_cotangent = centred(key_of[1], (TOKENS, D), 1.0, 6.0, ((0, 16),))
    recurrent_output = centred(key_of[2], (TOKENS, HW), 1.0, 6.0, ((0, 16), (1, 2)))
    forget_logit = centred(key_of[3], (TOKENS, HW), 2.0, 12.0, ((0, 16), (1, 2)))
    forget_cotangent = centred(key_of[4], (TOKENS, HW), 1.0, 6.0, ((0, 16), (1, 2)))
    lower_bound = jnp.clip(0.2 + 0.7 * jax.random.uniform(key_of[5], (HW,), jnp.float32) ** levels(key_of[5], (HW,), ((0, 2),), -0.2, 0.2), 0.2, 0.9)
    basis_in = draw_basis_in(jax.random.fold_in(key_of[14], 71), 0)
    basis_out = draw_basis_out(jax.random.fold_in(key_of[14], 71), 0)
    moment_in = centred(key_of[8], (R, HW), 1.0, 6.0, ((0, 16), (1, 2)), jnp.float32)
    second_in = jnp.clip(jnp.exp(math.log(4.0) - 2.7725887 * jax.random.uniform(key_of[9], (R, HW), jnp.float32) ** levels(key_of[9], (R, HW), ((0, 16), (1, 2)), -0.2, 0.2)), 0.25, 4.0)
    moment_out = centred(key_of[10], (R, HW), 1.0, 6.0, ((0, 16), (1, 2)), jnp.float32)
    second_out = jnp.clip(jnp.exp(math.log(4.0) - 2.7725887 * jax.random.uniform(key_of[11], (R, HW), jnp.float32) ** levels(key_of[11], (R, HW), ((0, 16), (1, 2)), -0.2, 0.2)), 0.25, 4.0)
    weight_in = centred(key_of[12], (D, HW), D ** -0.5, 0.109375, ((0, 16), (1, 2)), jnp.float32)
    weight_out = centred(key_of[13], (HW, D), HW ** -0.5, 0.15625, ((0, 2), (1, 16)), jnp.float32)
    return {"saved_input": saved_input, "output_cotangent": output_cotangent, "recurrent_output": recurrent_output, "forget_logit": forget_logit, "forget_cotangent": forget_cotangent, "lower_bound": lower_bound, "basis_in": basis_in, "basis_out": basis_out, "moment_in": moment_in, "second_in": second_in, "moment_out": moment_out, "second_out": second_out, "weight_in": weight_in, "weight_out": weight_out}


def reference(saved_input, output_cotangent, recurrent_output, forget_logit, forget_cotangent, lower_bound, basis_in, basis_out, moment_in, second_in, moment_out, second_out, weight_in, weight_out):
    sig = jax.nn.sigmoid(forget_logit.astype(jnp.float32))
    gate_cot = (forget_cotangent.astype(jnp.float32) * (1.0 - lower_bound)[None, :] * sig * (1.0 - sig)).astype(jnp.bfloat16)
    coded_in = jnp.dot(saved_input, basis_in, preferred_element_type=jnp.float32).astype(jnp.bfloat16)
    coded_out = jnp.dot(output_cotangent, basis_out, preferred_element_type=jnp.float32).astype(jnp.bfloat16)
    low_in = jnp.dot(coded_in.T, gate_cot, preferred_element_type=jnp.float32)
    low_out = jnp.dot(coded_out.T, recurrent_output, preferred_element_type=jnp.float32)
    total = jnp.sum(low_in * low_in) + jnp.sum(low_out * low_out)
    clip = jnp.minimum(1.0, jnp.sqrt(jnp.float32(2 * R * HW)) * lax.rsqrt(total + 1e-06))
    grad_in = clip * low_in
    grad_out = clip * low_out
    moment_in_new = 0.8 * moment_in + 0.2 * grad_in
    moment_out_new = 0.8 * moment_out + 0.2 * grad_out
    second_in_new = 0.9 * second_in + 0.1 * grad_in * grad_in
    second_out_new = 0.9 * second_out + 0.1 * grad_out * grad_out
    step_in = moment_in_new / (jnp.sqrt(second_in_new) + 1e-08)
    step_out = moment_out_new / (jnp.sqrt(second_out_new) + 1e-08)
    update_in = jnp.dot(basis_in.astype(jnp.float32), step_in, precision=lax.Precision.HIGHEST)
    update_out = jnp.dot(step_out.T, basis_out.astype(jnp.float32).T, precision=lax.Precision.HIGHEST)
    weight_in_new = weight_in - 0.01 * update_in
    weight_out_new = weight_out - 0.01 * update_out
    return (moment_in_new, second_in_new, moment_out_new, second_out_new, weight_in_new, weight_out_new, weight_in_new.astype(jnp.bfloat16), weight_out_new.astype(jnp.bfloat16))
```

```python
import functools

import jax
import jax.numpy as jnp
from jax import lax
from jax.experimental import pallas as pl
from jax.experimental.pallas import tpu as pltpu
from jax.sharding import PartitionSpec as P

MESH = pl.DeviceIdType.MESH
F32 = jnp.float32
BF16 = jnp.bfloat16
UNROLL = 16


def loop(start, stop, body):
    if stop - start <= UNROLL:
        for i in range(start, stop):
            body(i)
    else:

        @pl.loop(start, stop)
        def _(i):
            body(i)


def mod(value, n):
    return lax.rem(value + 2 * n, n)


def kernel(
    nf,
    nt,
    limit,
    x_hbm,
    y_hbm,
    rec_hbm,
    logit_hbm,
    fcot_hbm,
    lower_ref,
    basis_in_hbm,
    basis_out_hbm,
    m_in,
    s_in,
    m_out,
    s_out,
    w_in,
    w_out,
    mn_in,
    sn_in,
    mn_out,
    sn_out,
    wn_in,
    wn_out,
    copy_in,
    copy_out,
    x,
    y,
    rec,
    logit,
    fcot,
    bas_in,
    bas_out,
    gate,
    term,
    coded,
    part,
    peer,
    hop,
    step,
    flat,
    wb_in,
    wb_out,
    tots,
    load_sem,
    base_sem,
    send_sem,
    ring_a,
    ring_b,
    ring_d,
    ring_f,
    pair_sem,
    tot_sem,
):
    f = lax.axis_index("fs")
    tp = lax.axis_index("tp")
    n = nf // 2
    z = n // 2
    core = lax.rem(f, 2)
    chip = f // 2
    row, column = chip // 2, lax.rem(chip, 2)
    me = (1 - column) * row + column * (n - 1 - row)
    partner = (f + 1 - 2 * core, tp)

    def chip_at(position):
        side = position // z
        return 2 * ((1 - side) * position + side * (n - 1 - position)) + side

    def dev_at(position):
        return chip_at(position) * 2 + core

    ways = (1, -1)
    ahead = tuple((dev_at(mod(me + way, n)), tp) for way in ways)

    loads = [
        pltpu.make_async_copy(src, dst, load_sem.at[i])
        for i, (src, dst) in enumerate(
            ((logit_hbm, logit), (fcot_hbm, fcot), (x_hbm, x), (y_hbm, y), (rec_hbm, rec))
        )
    ]
    depth = basis_in_hbm.shape[0]
    cut = 2 if depth % 32 == 0 else 1
    piece = depth // cut

    def rows(ref, dev, c):
        return ref.at[pl.ds(pl.multiple_of(dev * depth + c * piece, piece), piece)]

    def own(ref, dev):
        return ref.at[pl.ds(pl.multiple_of(dev * depth, depth), depth)]

    own_loads = [
        pltpu.make_async_copy(basis_in_hbm, own(bas_in, f), base_sem.at[0]),
        pltpu.make_async_copy(basis_out_hbm, own(bas_out, f), base_sem.at[1]),
    ]
    for copy in own_loads + loads:
        copy.start()

    barrier = pltpu.get_barrier_semaphore()
    everyone = nf * nt
    my_id = f * nt + tp

    def other(i):
        target = lax.rem(my_id + i, everyone)
        return (target // nt, lax.rem(target, nt))

    @pl.loop(1, everyone)
    def _(i):
        pl.semaphore_signal(barrier, inc=1, device_id=other(i), device_id_type=MESH)

    pl.semaphore_wait(barrier, everyone - 1)

    def gather(view, chunks, ring_sem, phase, between=None):
        def ring_copy(t, s, c):
            block = view(t, dev_at(mod(me - ways[t] * s, n)), c)
            return pltpu.make_async_remote_copy(
                src_ref=block,
                dst_ref=block,
                send_sem=send_sem.at[phase, t, s, c],
                recv_sem=ring_sem.at[t, s, c],
                device_id=ahead[t],
                device_id_type=MESH,
            )

        def pair_copy(t, s, c):
            block = view(t, dev_at(mod(me - ways[t] * s, n)), c)
            return pltpu.make_async_remote_copy(
                src_ref=block,
                dst_ref=block,
                send_sem=pair_sem.at[phase, 0, t, s, c],
                recv_sem=pair_sem.at[phase, 1, t, s, c],
                device_id=partner,
                device_id_type=MESH,
            )

        both = [(t, c) for c in range(chunks) for t in range(2)]

        def stage(s, first=False, last=False):
            for t, c in both:
                if not first:
                    ring_copy(t, s - 1, c).wait_recv()
                if not last:
                    ring_copy(t, s, c).start()
                pair_copy(t, s, c).start()

        stage(0, first=True)
        if between is not None:
            between()
        loop(1, n - 1, stage)
        stage(n - 1, last=True)

        def finish(s):
            for t, c in both:
                pair_copy(t, s, c).wait()

        def sent(s):
            for t, c in both:
                ring_copy(t, s, c).wait_send()

        loop(0, n, finish)
        loop(0, n - 1, sent)

    def make_gate():
        loads[0].wait()
        loads[1].wait()
        tile = 64

        @pl.loop(0, gate.shape[0] // tile)
        def _(i):
            at = pl.ds(pl.multiple_of(i * tile, tile), tile)
            sig = jax.nn.sigmoid(logit[at].astype(F32))
            gate[at] = (
                fcot[at].astype(F32) * (1.0 - lower_ref[...]) * sig * (1.0 - sig)
            ).astype(BF16)

    for copy in own_loads:
        copy.wait()
    gather(lambda t, dev, c: rows((bas_in, bas_out)[t], dev, c), cut, ring_a, 0, make_gate)

    for copy in loads[2:]:
        copy.wait()
    units = gate.shape[1]
    span = part.shape[2]
    lanes = 2 if units % 256 == 0 else 1
    width = units // lanes

    for t, (data, basis, cot) in enumerate(((x, bas_in, gate), (y, bas_out, rec))):
        tile = 128

        @pl.loop(0, data.shape[0] // tile)
        def _(i):
            at = pl.ds(pl.multiple_of(i * tile, tile), tile)
            coded[at] = jnp.dot(data[at], basis[...], preferred_element_type=F32).astype(BF16)

        for c in range(lanes):
            at = slice(c * width, (c + 1) * width)
            term[:, at] = lax.dot_general(
                coded[...], cot[:, at], (((0,), (0,)), ((), ())), preferred_element_type=F32
            )
        for k in range(nf):
            part[t * 2 + k % 2, k // 2] = term[k * span : (k + 1) * span]

    def pair_sum(t):
        return pltpu.make_async_remote_copy(
            src_ref=part.at[t * 2 + 1 - core],
            dst_ref=peer.at[t],
            send_sem=pair_sem.at[3, 0, t, 0, 0],
            recv_sem=pair_sem.at[3, 1, t, 0, 0],
            device_id=partner,
            device_id_type=MESH,
        )

    for t in range(2):
        pair_sum(t).start()
    for t in range(2):
        pair_sum(t).wait_recv()

    def ring_add(t, s, c):
        at = pl.ds(c * width, width)
        return pltpu.make_async_remote_copy(
            src_ref=hop.at[t, s, :, at],
            dst_ref=hop.at[t, s + 1, :, at],
            send_sem=send_sem.at[3, t, s, c],
            recv_sem=ring_b.at[t, s, c],
            device_id=ahead[t],
            device_id_type=MESH,
        )

    both = [(t, c) for c in range(lanes) for t in range(2)]

    def mine(t, s, c):
        position = mod(me - ways[t] * (s + 1), n)
        at = pl.ds(c * width, width)
        place = chip_at(position)
        return part[t * 2 + core, place, :, at] + peer[t, place, :, at]

    def add_stage(s):
        for t, c in both:
            at = pl.ds(c * width, width)
            ring_add(t, s - 1, c).wait_recv()
            hop[t, s, :, at] = hop[t, s, :, at] + mine(t, s, c)
            ring_add(t, s, c).start()

    for t, c in both:
        at = pl.ds(c * width, width)
        hop[t, 0, :, at] = mine(t, 0, c)
        ring_add(t, 0, c).start()
    loop(1, n - 1, add_stage)
    for t, c in both:
        at = pl.ds(c * width, width)
        ring_add(t, n - 2, c).wait_recv()
        hop[t, n - 1, :, at] = hop[t, n - 1, :, at] + mine(t, n - 1, c)

    low = [hop[t, n - 1] for t in range(2)]
    square = jnp.sum(low[0] * low[0] + low[1] * low[1], axis=(0, 1), keepdims=True)
    tots[my_id] = jnp.broadcast_to(square, tots.shape[1:])

    def tell(i):
        return pltpu.make_async_remote_copy(
            src_ref=tots.at[my_id],
            dst_ref=tots.at[my_id],
            send_sem=tot_sem.at[0],
            recv_sem=tot_sem.at[1],
            device_id=other(i),
            device_id_type=MESH,
        )

    @pl.loop(1, everyone)
    def _(i):
        tell(i).start()

    def sent_adds(s):
        for t, c in both:
            ring_add(t, s, c).wait_send()

    loop(0, n - 1, sent_adds)
    for t in range(2):
        pair_sum(t).wait_send()
    all_tots = tots.at[pl.ds(0, everyone - 1)]
    pltpu.make_async_copy(all_tots, all_tots, tot_sem.at[1]).wait()
    pltpu.make_async_copy(all_tots, all_tots, tot_sem.at[0]).wait()

    total = jnp.sum(tots[...], axis=0)
    clip = jnp.minimum(1.0, jnp.sqrt(F32(limit)) * lax.rsqrt(total + 1e-06))[0:1, 0:1]
    for t, (m, s2, mn, sn) in enumerate(
        ((m_in, s_in, mn_in, sn_in), (m_out, s_out, mn_out, sn_out))
    ):
        grad = clip * hop[t, n - 1]
        moment = 0.8 * m[...] + 0.2 * grad
        second = 0.9 * s2[...] + 0.1 * grad * grad
        mn[...] = moment
        sn[...] = second
        step[t, f] = moment / (jnp.sqrt(second) + 1e-08)

    gather(
        lambda t, dev, c: step.at[t, dev, :, pl.ds(c * width, width)], lanes, ring_d, 1
    )

    for t, (basis, w, wn, wb) in enumerate(
        ((bas_in, w_in, wn_in, wb_in), (bas_out, w_out, wn_out, wb_out))
    ):
        for k in range(nf):
            flat[k * span : (k + 1) * span] = step[t, k]
        whole = flat[...]
        high = whole.astype(BF16)
        rest = (whole - high.astype(F32)).astype(BF16)
        mat = own(basis, f)[...]
        update = jnp.dot(mat, rest, preferred_element_type=F32) + jnp.dot(
            mat, high, preferred_element_type=F32
        )
        new = w[...] - 0.01 * update
        wn[...] = new
        wb[...] = new.astype(BF16)

    puts = [
        pltpu.make_async_copy(wb_in, own(copy_in, f), base_sem.at[0]),
        pltpu.make_async_copy(wb_out, own(copy_out, f), base_sem.at[1]),
    ]
    for copy in puts:
        copy.start()
    for copy in puts:
        copy.wait()
    gather(lambda t, dev, c: rows((copy_in, copy_out)[t], dev, c), cut, ring_f, 2)


def body(
    saved_input,
    output_cotangent,
    recurrent_output,
    forget_logit,
    forget_cotangent,
    lower_bound,
    basis_in,
    basis_out,
    moment_in,
    second_in,
    moment_out,
    second_out,
    weight_in,
    weight_out,
):
    nf, nt = lax.axis_size("fs"), lax.axis_size("tp")
    n = nf // 2
    tokens, model = saved_input.shape
    units = recurrent_output.shape[1]
    depth, rank = basis_in.shape
    span = moment_in.shape[0]
    limit = 2.0 * rank * units * nt
    small = jax.ShapeDtypeStruct((span, units), F32)
    weight = jax.ShapeDtypeStruct((depth, units), F32)
    copied = jax.ShapeDtypeStruct((model, units), BF16)
    cut = 2 if depth % 32 == 0 else 1
    lanes = 2 if units % 256 == 0 else 1
    most = max(cut, lanes)
    hbm = pl.BlockSpec(memory_space=pl.ANY)
    vmem = pl.BlockSpec(memory_space=pltpu.VMEM)
    dma = pltpu.SemaphoreType.DMA
    outs = pl.pallas_call(
        functools.partial(kernel, nf, nt, limit),
        out_shape=(small, small, small, small, weight, weight, copied, copied),
        in_specs=[hbm] * 5 + [vmem] + [hbm] * 2 + [vmem] * 6,
        out_specs=[vmem] * 6 + [hbm] * 2,
        scratch_shapes=[
            pltpu.VMEM((tokens, model), BF16),
            pltpu.VMEM((tokens, model), BF16),
            pltpu.VMEM((tokens, units), BF16),
            pltpu.VMEM((tokens, units), BF16),
            pltpu.VMEM((tokens, units), BF16),
            pltpu.VMEM((model, rank), BF16),
            pltpu.VMEM((model, rank), BF16),
            pltpu.VMEM((tokens, units), BF16),
            pltpu.VMEM((rank, units), F32),
            pltpu.VMEM((tokens, rank), BF16),
            pltpu.VMEM((4, n, span, units), F32),
            pltpu.VMEM((2, n, span, units), F32),
            pltpu.VMEM((2, n, span, units), F32),
            pltpu.VMEM((2, nf, span, units), F32),
            pltpu.VMEM((rank, units), F32),
            pltpu.VMEM((depth, units), BF16),
            pltpu.VMEM((depth, units), BF16),
            pltpu.VMEM((nf * nt, 8, 128), F32),
            dma((5,)),
            dma((2,)),
            dma((4, 2, n - 1, most)),
            dma((2, n - 1, cut)),
            dma((2, n - 1, lanes)),
            dma((2, n - 1, lanes)),
            dma((2, n - 1, cut)),
            dma((4, 2, 2, n, most)),
            dma((2,)),
        ],
        compiler_params=pltpu.CompilerParams(
            collective_id=0, has_side_effects=True, vmem_limit_bytes=60 * 1024 * 1024
        ),
    )(
        saved_input,
        output_cotangent,
        recurrent_output,
        forget_logit,
        forget_cotangent,
        lower_bound[None, :],
        basis_in,
        basis_out,
        moment_in,
        second_in,
        moment_out,
        second_out,
        weight_in,
        weight_out.T,
    )
    return outs[:5] + (outs[5].T, outs[6], outs[7].T)


def solution(mesh):
    return jax.shard_map(
        body,
        mesh=mesh,
        in_specs=(
            P("fs", None),
            P("fs", None),
            P("fs", "tp"),
            P("fs", "tp"),
            P("fs", "tp"),
            P("tp"),
            P("fs", None),
            P("fs", None),
            P("fs", "tp"),
            P("fs", "tp"),
            P("fs", "tp"),
            P("fs", "tp"),
            P("fs", "tp"),
            P("tp", "fs"),
        ),
        out_specs=(
            P("fs", "tp"),
            P("fs", "tp"),
            P("fs", "tp"),
            P("fs", "tp"),
            P("fs", "tp"),
            P("tp", "fs"),
            P(None, "tp"),
            P("tp", None),
        ),
        check_vma=False,
    )
```

```python
import functools

import jax
import jax.numpy as jnp
from jax import lax
from jax.experimental import pallas as pl
from jax.experimental.pallas import tpu as pltpu
from jax.sharding import PartitionSpec as P

MESH = pl.DeviceIdType.MESH
F32 = jnp.float32
BF16 = jnp.bfloat16
UNROLL = 16


def loop(start, stop, body):
    if stop - start <= UNROLL:
        for i in range(start, stop):
            body(i)
    else:

        @pl.loop(start, stop)
        def _(i):
            body(i)


def mod(value, n):
    return lax.rem(value + 2 * n, n)


def kernel(
    nf,
    nt,
    limit,
    x_hbm,
    y_hbm,
    rec_hbm,
    logit_hbm,
    fcot_hbm,
    lower_ref,
    basis_in_hbm,
    basis_out_hbm,
    m_in,
    s_in,
    m_out,
    s_out,
    w_in,
    w_out,
    mn_in,
    sn_in,
    mn_out,
    sn_out,
    wn_in,
    wn_out,
    copy_in,
    copy_out,
    x,
    y,
    rec,
    logit,
    fcot,
    bas_in,
    bas_out,
    gate,
    term,
    coded,
    part,
    peer,
    hop,
    step,
    flat,
    wb_in,
    wb_out,
    tots,
    load_sem,
    base_sem,
    send_sem,
    ring_a,
    ring_b,
    ring_d,
    ring_f,
    pair_sem,
    sum_sem,
    tot_sem,
):
    f = lax.axis_index("fs")
    tp = lax.axis_index("tp")
    n = nf // 2
    z = n // 2
    core = lax.rem(f, 2)
    chip = f // 2
    row, column = chip // 2, lax.rem(chip, 2)
    me = (1 - column) * row + column * (n - 1 - row)
    partner = (f + 1 - 2 * core, tp)

    def chip_at(position):
        side = position // z
        return 2 * ((1 - side) * position + side * (n - 1 - position)) + side

    def dev_at(position):
        return chip_at(position) * 2 + core

    loads = [
        pltpu.make_async_copy(src, dst, load_sem.at[i])
        for i, (src, dst) in enumerate(
            ((logit_hbm, logit), (fcot_hbm, fcot), (x_hbm, x), (y_hbm, y), (rec_hbm, rec))
        )
    ]
    depth = basis_in_hbm.shape[0]
    cut = 2 if depth % 32 == 0 else 1
    piece = depth // cut

    def rows(ref, dev, c):
        return ref.at[pl.ds(pl.multiple_of(dev * depth + c * piece, piece), piece)]

    def own(ref, dev):
        return ref.at[pl.ds(pl.multiple_of(dev * depth, depth), depth)]

    own_loads = [
        pltpu.make_async_copy(basis_in_hbm, own(bas_in, f), base_sem.at[0]),
        pltpu.make_async_copy(basis_out_hbm, own(bas_out, f), base_sem.at[1]),
    ]
    for copy in own_loads + loads:
        copy.start()

    barrier = pltpu.get_barrier_semaphore()
    everyone = nf * nt
    my_id = f * nt + tp

    def other(i):
        target = lax.rem(my_id + i, everyone)
        return (target // nt, lax.rem(target, nt))

    @pl.loop(1, everyone)
    def _(i):
        pl.semaphore_signal(barrier, inc=1, device_id=other(i), device_id_type=MESH)

    pl.semaphore_wait(barrier, everyone - 1)

    far = n // 2
    near = n - 1 - far
    one_way = ((0, 1, n - 1), (1, -1, n - 1))
    two_way = ((0, 1, far), (1, -1, far), (0, -1, near), (1, 1, near))

    def neighbour(way):
        return (dev_at(mod(me + way, n)), tp)

    def gather(flows, view, chunks, ring_sem, phase, between=None):
        stride = flows[0][2]

        def remote(j, s, c, sems, target):
            t, way, _ = flows[j]
            block = view(t, dev_at(mod(me - way * s, n)), c)
            return pltpu.make_async_remote_copy(
                src_ref=block,
                dst_ref=block,
                send_sem=sems[0],
                recv_sem=sems[1],
                device_id=target,
                device_id_type=MESH,
            )

        def ring_copy(j, s, c):
            sems = send_sem.at[phase, j * stride + s, c], ring_sem.at[j, s, c]
            return remote(j, s, c, sems, neighbour(flows[j][1]))

        def pair_copy(j, s, c):
            at = j * (stride + 1) + s
            sems = pair_sem.at[phase, 0, at, c], pair_sem.at[phase, 1, at, c]
            return remote(j, s, c, sems, partner)

        def each(s, act):
            for c in range(chunks):
                for j in range(len(flows)):
                    act(j, s, c)

        def move(j, s, c, first=False, last=False):
            if not first:
                ring_copy(j, s - 1, c).wait_recv()
            if not last:
                ring_copy(j, s, c).start()
            if not first or j < 2:
                pair_copy(j, s, c).start()

        least = min(hops for _, _, hops in flows)
        most = max(hops for _, _, hops in flows)
        each(0, functools.partial(move, first=True))
        if between is not None:
            between()
        loop(1, least, lambda s: each(s, move))
        for s in range(least, most + 1):
            for c in range(chunks):
                for j, (_, _, hops) in enumerate(flows):
                    if s <= hops:
                        move(j, s, c, last=s == hops)

        def finish(j, s, c):
            pair_copy(j, s, c).wait()

        def sent(j, s, c):
            ring_copy(j, s, c).wait_send()

        for c in range(chunks):
            for j, (_, _, hops) in enumerate(flows):
                if j < 2:
                    finish(j, 0, c)
                for s in range(least, hops):
                    sent(j, s, c)
                for s in range(least, hops + 1):
                    finish(j, s, c)
        loop(1, least, lambda s: each(s, finish))
        loop(0, least, lambda s: each(s, sent))

    def make_gate():
        loads[0].wait()
        loads[1].wait()
        tile = 64

        @pl.loop(0, gate.shape[0] // tile)
        def _(i):
            at = pl.ds(pl.multiple_of(i * tile, tile), tile)
            sig = jax.nn.sigmoid(logit[at].astype(F32))
            gate[at] = (
                fcot[at].astype(F32) * (1.0 - lower_ref[...]) * sig * (1.0 - sig)
            ).astype(BF16)

    for copy in own_loads:
        copy.wait()
    gather(
        one_way,
        lambda t, dev, c: rows((bas_in, bas_out)[t], dev, c),
        cut,
        ring_a,
        0,
        make_gate,
    )

    for copy in loads[2:]:
        copy.wait()
    units = gate.shape[1]
    span = part.shape[2]
    lanes = 2 if units % 256 == 0 else 1
    width = units // lanes

    def encode(data, basis):
        tile = 128

        @pl.loop(0, data.shape[0] // tile)
        def _(i):
            at = pl.ds(pl.multiple_of(i * tile, tile), tile)
            coded[at] = jnp.dot(data[at], basis[...], preferred_element_type=F32).astype(BF16)

    def project(t, cot):
        for c in range(lanes):
            at = slice(c * width, (c + 1) * width)
            term[:, at] = lax.dot_general(
                coded[...], cot[:, at], (((0,), (0,)), ((), ())), preferred_element_type=F32
            )
        for k in range(nf):
            part[t * 2 + k % 2, k // 2] = term[k * span : (k + 1) * span]

    def pair_sum(t):
        return pltpu.make_async_remote_copy(
            src_ref=part.at[t * 2 + 1 - core],
            dst_ref=peer.at[t],
            send_sem=sum_sem.at[0, t],
            recv_sem=sum_sem.at[1, t],
            device_id=partner,
            device_id_type=MESH,
        )

    def ring_add(j, s, c):
        at = pl.ds(c * width, width)
        return pltpu.make_async_remote_copy(
            src_ref=hop.at[j, s, :, at],
            dst_ref=hop.at[j, s + 1, :, at],
            send_sem=send_sem.at[3, j * far + s, c],
            recv_sem=ring_b.at[j, s, c],
            device_id=neighbour(two_way[j][1]),
            device_id_type=MESH,
        )

    def mine(j, s, c):
        t, way, hops = two_way[j]
        at = pl.ds(c * width, width)
        place = chip_at(mod(me + way * (hops - s), n))
        return part[t * 2 + core, place, :, at] + peer[t, place, :, at]

    def begin(t):
        pair_sum(t).wait_recv()
        for c in range(lanes):
            at = pl.ds(c * width, width)
            for j in (t, t + 2):
                if two_way[j][2] > 0:
                    hop[j, 0, :, at] = mine(j, 0, c)
                    ring_add(j, 0, c).start()

    def relay(j, s, c):
        at = pl.ds(c * width, width)
        ring_add(j, s - 1, c).wait_recv()
        hop[j, s, :, at] = hop[j, s, :, at] + mine(j, s, c)
        ring_add(j, s, c).start()

    def flows_do(act, s, which=range(4)):
        for c in range(lanes):
            for j in which:
                act(j, s, c)

    encode(x, bas_in)
    project(0, gate)
    pair_sum(0).start()
    encode(y, bas_out)
    begin(0)
    project(1, rec)
    pair_sum(1).start()
    begin(1)
    loop(1, near, lambda s: flows_do(relay, s))
    flows_do(relay, far - 1, range(2))
    for c in range(lanes):
        for t in range(2):
            at = pl.ds(c * width, width)
            ring_add(t + 2, near - 1, c).wait_recv()
            hop[t + 2, near, :, at] = hop[t + 2, near, :, at] + mine(t + 2, near, c)
    for c in range(lanes):
        for t in range(2):
            at = pl.ds(c * width, width)
            ring_add(t, far - 1, c).wait_recv()
            hop[t, far, :, at] = hop[t, far, :, at] + hop[t + 2, near, :, at]

    low = [hop[t, far] for t in range(2)]
    square = jnp.sum(low[0] * low[0] + low[1] * low[1], axis=(0, 1), keepdims=True)
    tots[my_id] = jnp.broadcast_to(square, tots.shape[1:])

    def tell(i):
        return pltpu.make_async_remote_copy(
            src_ref=tots.at[my_id],
            dst_ref=tots.at[my_id],
            send_sem=tot_sem.at[0],
            recv_sem=tot_sem.at[1],
            device_id=other(i),
            device_id_type=MESH,
        )

    @pl.loop(1, everyone)
    def _(i):
        tell(i).start()

    def sent_add(j, s, c):
        ring_add(j, s, c).wait_send()

    loop(0, near, lambda s: flows_do(sent_add, s))
    flows_do(sent_add, far - 1, range(2))
    for t in range(2):
        pair_sum(t).wait_send()
    all_tots = tots.at[pl.ds(0, everyone - 1)]
    pltpu.make_async_copy(all_tots, all_tots, tot_sem.at[1]).wait()
    pltpu.make_async_copy(all_tots, all_tots, tot_sem.at[0]).wait()

    total = jnp.sum(tots[...], axis=0)
    clip = jnp.minimum(1.0, jnp.sqrt(F32(limit)) * lax.rsqrt(total + 1e-06))[0:1, 0:1]
    for t, (m, s2, mn, sn) in enumerate(
        ((m_in, s_in, mn_in, sn_in), (m_out, s_out, mn_out, sn_out))
    ):
        grad = clip * hop[t, far]
        moment = 0.8 * m[...] + 0.2 * grad
        second = 0.9 * s2[...] + 0.1 * grad * grad
        mn[...] = moment
        sn[...] = second
        step[t, f] = moment / (jnp.sqrt(second) + 1e-08)

    gather(
        two_way,
        lambda t, dev, c: step.at[t, dev, :, pl.ds(c * width, width)],
        lanes,
        ring_d,
        1,
    )

    for t, (basis, w, wn, wb) in enumerate(
        ((bas_in, w_in, wn_in, wb_in), (bas_out, w_out, wn_out, wb_out))
    ):
        for k in range(nf):
            flat[k * span : (k + 1) * span] = step[t, k]
        whole = flat[...]
        high = whole.astype(BF16)
        rest = (whole - high.astype(F32)).astype(BF16)
        mat = own(basis, f)[...]
        update = jnp.dot(mat, rest, preferred_element_type=F32) + jnp.dot(
            mat, high, preferred_element_type=F32
        )
        new = w[...] - 0.01 * update
        wn[...] = new
        wb[...] = new.astype(BF16)

    puts = [
        pltpu.make_async_copy(wb_in, own(copy_in, f), base_sem.at[0]),
        pltpu.make_async_copy(wb_out, own(copy_out, f), base_sem.at[1]),
    ]
    for copy in puts:
        copy.start()
    for copy in puts:
        copy.wait()
    gather(
        one_way, lambda t, dev, c: rows((copy_in, copy_out)[t], dev, c), cut, ring_f, 2
    )


def settle(*refs):
    ins, outs = refs[:8], refs[8:]

    @pl.when(pl.program_id(0) == 0)
    def _():
        for src, dst in zip(ins[:6], outs[:6]):
            dst[...] = src[...]

    outs[6][...] = ins[6][...]
    outs[7][...] = ins[7][...].T


def body(
    saved_input,
    output_cotangent,
    recurrent_output,
    forget_logit,
    forget_cotangent,
    lower_bound,
    basis_in,
    basis_out,
    moment_in,
    second_in,
    moment_out,
    second_out,
    weight_in,
    weight_out,
):
    nf, nt = lax.axis_size("fs"), lax.axis_size("tp")
    n = nf // 2
    tokens, model = saved_input.shape
    units = recurrent_output.shape[1]
    depth, rank = basis_in.shape
    span = moment_in.shape[0]
    limit = 2.0 * rank * units * nt
    small = jax.ShapeDtypeStruct((span, units), F32)
    weight = jax.ShapeDtypeStruct((depth, units), F32)
    copied = jax.ShapeDtypeStruct((model, units), BF16)
    cut = 2 if depth % 32 == 0 else 1
    lanes = 2 if units % 256 == 0 else 1
    most = max(cut, lanes)
    hbm = pl.BlockSpec(memory_space=pl.ANY)
    vmem = pl.BlockSpec(memory_space=pltpu.VMEM)
    dma = pltpu.SemaphoreType.DMA
    outs = pl.pallas_call(
        functools.partial(kernel, nf, nt, limit),
        out_shape=(small, small, small, small, weight, weight, copied, copied),
        in_specs=[hbm] * 5 + [vmem] + [hbm] * 2 + [vmem] * 6,
        out_specs=[vmem] * 6 + [hbm] * 2,
        scratch_shapes=[
            pltpu.VMEM((tokens, model), BF16),
            pltpu.VMEM((tokens, model), BF16),
            pltpu.VMEM((tokens, units), BF16),
            pltpu.VMEM((tokens, units), BF16),
            pltpu.VMEM((tokens, units), BF16),
            pltpu.VMEM((model, rank), BF16),
            pltpu.VMEM((model, rank), BF16),
            pltpu.VMEM((tokens, units), BF16),
            pltpu.VMEM((rank, units), F32),
            pltpu.VMEM((tokens, rank), BF16),
            pltpu.VMEM((4, n, span, units), F32),
            pltpu.VMEM((2, n, span, units), F32),
            pltpu.VMEM((4, n // 2 + 1, span, units), F32),
            pltpu.VMEM((2, nf, span, units), F32),
            pltpu.VMEM((rank, units), F32),
            pltpu.VMEM((depth, units), BF16),
            pltpu.VMEM((depth, units), BF16),
            pltpu.VMEM((nf * nt, 8, 128), F32),
            dma((5,)),
            dma((2,)),
            dma((4, 2 * n, most)),
            dma((2, n - 1, cut)),
            dma((4, n // 2, lanes)),
            dma((4, n // 2 + 1, lanes)),
            dma((2, n - 1, cut)),
            dma((3, 2, 2 * n + 4, most)),
            dma((2, 2)),
            dma((2,)),
        ],
        compiler_params=pltpu.CompilerParams(
            collective_id=0, has_side_effects=True, vmem_limit_bytes=60 * 1024 * 1024
        ),
    )(
        saved_input,
        output_cotangent,
        recurrent_output,
        forget_logit,
        forget_cotangent,
        lower_bound[None, :],
        basis_in,
        basis_out,
        moment_in,
        second_in,
        moment_out,
        second_out,
        weight_in,
        weight_out.T,
    )
    blocks = 8 if model % 1024 == 0 else 1
    rows = model // blocks
    tall = pl.BlockSpec((rows, units), lambda i: (i, 0))
    kept = [pl.BlockSpec(o.shape, lambda i: (0, 0)) for o in outs[:6]]
    outs = pl.pallas_call(
        settle,
        grid=(blocks,),
        out_shape=(small, small, small, small, weight, weight, copied)
        + (jax.ShapeDtypeStruct((units, model), BF16),),
        in_specs=kept + [tall, tall],
        out_specs=kept + [tall, pl.BlockSpec((units, rows), lambda i: (0, i))],
        compiler_params=pltpu.CompilerParams(dimension_semantics=("arbitrary",)),
    )(*outs)
    return tuple(outs[:5]) + (outs[5].T, outs[6], outs[7])


def solution(mesh):
    return jax.shard_map(
        body,
        mesh=mesh,
        in_specs=(
            P("fs", None),
            P("fs", None),
            P("fs", "tp"),
            P("fs", "tp"),
            P("fs", "tp"),
            P("tp"),
            P("fs", None),
            P("fs", None),
            P("fs", "tp"),
            P("fs", "tp"),
            P("fs", "tp"),
            P("fs", "tp"),
            P("fs", "tp"),
            P("tp", "fs"),
        ),
        out_specs=(
            P("fs", "tp"),
            P("fs", "tp"),
            P("fs", "tp"),
            P("fs", "tp"),
            P("fs", "tp"),
            P("tp", "fs"),
            P(None, "tp"),
            P("tp", None),
        ),
        check_vma=False,
    )
```
